32 devices in a mesh: grp: 2 (over x), ep: 16 (over z, y, core).
Axes of the slice: x: 2, y: 2, z: 4, core: 2. Of those that a mesh axis runs over, the one named last changes fastest.
Arguments:
- stream: bfloat16 [32, 2048], P('grp', 'ep'), parts along dimension 0, may hold values from -48 to 48
- conv_cache: bfloat16 [32, 3, 2560], P(('grp', 'ep')), parts along dimension 0, may hold values from -6 to 6
- scan_state: float32 [32, 32, 64, 128], P(('grp', 'ep')), parts along dimension 0, may hold values from -4 to 4
- gate_weight: bfloat16 [2048, 2048], P('ep'), may hold values from -0.125 to 0.125
- value_weight: bfloat16 [2048, 2048], P('ep'), may hold values from -0.125 to 0.125
- entry_weight: bfloat16 [2048, 256], P('ep'), may hold values from -0.125 to 0.125
- readout_weight: bfloat16 [2048, 256], P('ep'), may hold values from -0.125 to 0.125
- step_weight: bfloat16 [2048, 32], P('ep'), may hold values from -0.125 to 0.125
- conv_weight: bfloat16 [4, 2560], replicated, may hold values from -3 to 3
- step_bias: float32 [32], replicated, may hold values from -4 to -1
- decay_rate: float32 [32], replicated, may hold values from 0.5 to 8
- skip_gain: float32 [32], replicated, may hold values from 0.1 to 1.9
- group_gain: float32 [2048], replicated, may hold values from 0.1 to 1.9
- out_weight: bfloat16 [2048, 2048], P(None, 'ep'), may hold values from -0.125 to 0.125
- first_gain: float32 [2048], replicated, may hold values from 0.1 to 1.9
- routes: int32 [32, 4], P('grp'), parts along dimension 0, may hold values from 0 to 15, all different within a row; in each aligned block of 16 rows (0 to 15, 16 to 31, ...) at most 8 rows name the same one
- route_weight: float32 [32, 4], P('grp'), parts along dimension 0, may hold values from 0.1 to 1
- expert_gate: bfloat16 [16, 2048, 256], P('ep'), may hold values from -0.125 to 0.125
- expert_up: bfloat16 [16, 2048, 256], P('ep'), may hold values from -0.125 to 0.125
- expert_down: bfloat16 [16, 256, 2048], P('ep'), may hold values from -0.375 to 0.375
- shared_gate: bfloat16 [2048, 256], replicated, may hold values from -0.125 to 0.125
- shared_up: bfloat16 [2048, 256], replicated, may hold values from -0.125 to 0.125
- shared_down: bfloat16 [256, 2048], replicated, may hold values from -0.375 to 0.375
- second_gain: float32 [2048], P('ep'), may hold values from 0.1 to 1.9
Outputs:
- result: bfloat16 [32, 2048], P('grp', 'ep'), parts along dimension 0
- new_conv: bfloat16 [32, 3, 2560], P(('grp', 'ep')), parts along dimension 0
- new_state: float32 [32, 32, 64, 128], P(('grp', 'ep')), parts along dimension 0
The draws below stay inside these ranges and needn't reach their ends.
There are 2 independent parts, one for each index of `grp`. The reference program is written for one: setup_inputs(seed, part) draws one part's arguments, and reference() takes and returns one part's arrays. A program takes and returns all parts, laid end to end along the dimension named above; an argument that names none is the same for every part. Nothing has to cross between parts.
Inputs may be any that keep to these rules, and one draw needn't show every extreme that they name: `routes`: each row names 4 different experts; no expert is named by more than 8 rows, a bound that some block reaches.
All inputs are finite; a program needn't handle non-finite values.
Results may differ from the reference program's by a relative error of at most 0.0065.
Values may be sent and summed in bfloat16 or wider, within the bound.
A program may use at most 64 MiB of HBM per device.

```python
import math
import jax
import jax.numpy as jnp
import numpy as np
from jax import lax

D = 2048
HEADS = 32
HEAD_DIM = 64
STATE = 128
GROUPS = 2
CONV = 4
EFF = 256
SFF = 256
TOPK = 4
TOKENS = 16
EXPERTS = 16
CAP = 8
INNER = 2048
KCONV = 2560


def draw_stream(key, part):
    column_scale = jnp.exp(jnp.linspace(0.0, jnp.log(3.0), D)).astype(jnp.float32)[None, :]
    values = jnp.clip(jax.random.normal(key, (TOKENS, D), jnp.float32), -6.0, 6.0) * column_scale
    return values.astype(jnp.bfloat16)


def level_of(own_key, extent, cuts, least, top_value):
    def one(dim, blocks):
        steps = jax.random.uniform(jax.random.fold_in(jax.random.fold_in(own_key, 6), dim), (blocks,), jnp.float32, least / len(cuts), top_value / len(cuts))
        return jnp.repeat(jnp.exp(steps), extent[dim] // blocks).reshape((-1,) + (1,) * (len(extent) - dim - 1))

    loudness = one(*cuts[0])
    for cut in cuts[1:]:
        loudness = loudness * one(*cut)
    return loudness


def deal_out(rng, own, number, rows, count, top, limit, slope):
    sequence = jax.random.permutation(rng, count)
    crowded, ordinary = load_shares(count, rows * top, limit, slope, True), load_shares(count, rows * top, limit, slope, False)
    places = jnp.arange(count)

    def named(tallies, offset_by):
        used = int((tallies > 0).sum())
        fixed = max(1, used // 4)
        shifted = fixed + (places - fixed + offset_by * (used - fixed)) % max(1, count - fixed)
        return jnp.zeros((count,), jnp.int32).at[sequence[jnp.where(places < fixed, places, shifted)]].set(jnp.asarray(tallies, jnp.int32))

    tallies = jnp.where(number % 4 == 0, named(crowded, number // 4), named(ordinary, number - number // 4 - 1))
    mixed = jax.random.permutation(jax.random.fold_in(own, 3), count)
    donor, sink = mixed[0:count // 2 * 2:2], mixed[1:count // 2 * 2:2]
    room = jnp.minimum(tallies[donor] - 1, limit - tallies[sink]) // 2
    room = jnp.where((donor == sequence[0]) | (sink == sequence[0]) | (tallies[sink] == 0), 0, jnp.maximum(room, 0))
    shifted = jax.random.randint(jax.random.fold_in(own, 4), (count // 2,), 0, 1 << 20) % (room + 1)
    tallies = tallies.at[donor].add(-shifted).at[sink].add(shifted)
    items = jnp.searchsorted(jnp.cumsum(tallies), jnp.arange(rows * top), side="right").astype(jnp.int32)
    table = items.reshape(top, rows).T
    table = table[jax.random.permutation(jax.random.fold_in(own, 1), rows)]
    offset_by = jax.random.randint(jax.random.fold_in(own, 2), (rows, 1), 0, top)
    return jnp.take_along_axis(table, (jnp.arange(top)[None, :] + offset_by) % top, axis=1)


def load_shares(count, total, limit, slope, full):
    weights = [(1 << 20) // math.isqrt(standing ** slope) + 1 for standing in range(1, count + 1)]
    largest = limit if full else min(limit, max(-(-total // count), total * weights[0] // sum(weights)))
    least = 1 if total - largest >= count - 1 else 0
    holding, surplus = [largest] + [least] * (count - 1), total - largest - least * (count - 1)
    while surplus > 0:
        movable = [i for i in range(1, count) if holding[i] < largest] or [i for i in range(1, count) if holding[i] < limit]
        whole, budget = sum([weights[i] for i in movable]), surplus
        for i in movable:
            more = min(limit - holding[i], max(1, budget * weights[i] // whole), surplus)
            holding[i] = holding[i] + more
            surplus = surplus - more
    return np.array(holding)


def normal_values(stream_key, dims, spread, limit, cuts=(), held_as=jnp.bfloat16):
    entries = jax.random.normal(stream_key, dims, jnp.float32) * spread
    if len(cuts) > 0:
        entries = level_of(stream_key, dims, cuts, -0.22, 0.18) * entries
    return jnp.clip(entries, min=-limit, max=limit).astype(held_as)


def setup_inputs(seed: int = 0, part: int = 0) -> dict:
    splits = jax.random.split(jax.random.key(seed), 25)
    part_keys = jax.random.split(jax.random.fold_in(splits[24], part), 25)
    stream = draw_stream(jax.random.fold_in(jax.random.fold_in(splits[24], part), 71), part)
    conv_cache = normal_values(part_keys[1], (TOKENS, CONV - 1, KCONV), 1.0, 6.0, ((0, 16),))
    scan_state = normal_values(part_keys[2], (TOKENS, HEADS, HEAD_DIM, STATE), 0.3, 4.0, ((0, 16),), jnp.float32)
    gate_weight = normal_values(splits[3], (D, INNER), D ** -0.5, 0.125, ((0, 16),))
    value_weight = normal_values(splits[4], (D, INNER), D ** -0.5, 0.125, ((0, 16),))
    entry_weight = normal_values(splits[5], (D, GROUPS * STATE), D ** -0.5, 0.125, ((0, 16),))
    readout_weight = normal_values(splits[6], (D, GROUPS * STATE), D ** -0.5, 0.125, ((0, 16),))
    step_weight = normal_values(splits[7], (D, HEADS), D ** -0.5, 0.125, ((0, 16),))
    conv_weight = normal_values(splits[8], (CONV, KCONV), 0.5, 3.0)
    step_bias = jnp.clip(jax.random.uniform(splits[9], (HEADS,), jnp.float32, -4.0, -1.0), -4.0, -1.0)
    decay_rate = jnp.clip(jnp.exp(jax.random.uniform(splits[10], (HEADS,), jnp.float32, math.log(0.5), math.log(8.0))), 0.5, 8.0)
    skip_gain = jnp.clip(1.0 + 0.18 * jax.random.normal(splits[11], (HEADS,), jnp.float32), 0.1, 1.9)
    group_gain = jnp.clip(1.0 + 0.18 * jax.random.normal(splits[12], (INNER,), jnp.float32), 0.1, 1.9)
    out_weight = normal_values(splits[13], (INNER, D), INNER ** -0.5, 0.125, ((1, 16),))
    first_gain = jnp.clip(1.0 + 0.18 * jax.random.normal(splits[14], (D,), jnp.float32), 0.1, 1.9)
    routes_keys = jax.random.split(jax.random.fold_in(part_keys[15], 1), TOKENS // TOKENS)
    routes_turns = jax.random.permutation(jax.random.fold_in(part_keys[15], 3), TOKENS // TOKENS)
    routes = jax.vmap(lambda own, number: deal_out(jax.random.fold_in(part_keys[15], 2), own, number, TOKENS, EXPERTS, TOPK, CAP, 2))(routes_keys, routes_turns).reshape((TOKENS, TOPK))
    route_weight = jnp.clip(jnp.exp(jax.random.uniform(part_keys[16], (TOKENS, TOPK), jnp.float32, math.log(0.1), math.log(1.0))), 0.1, 1.0)
    expert_gate = normal_values(splits[17], (EXPERTS, D, EFF), D ** -0.5, 0.125, ((0, 16),))
    expert_up = normal_values(splits[18], (EXPERTS, D, EFF), D ** -0.5, 0.125, ((0, 16),))
    expert_down = normal_values(splits[19], (EXPERTS, EFF, D), EFF ** -0.5, 0.375, ((0, 16),))
    shared_gate = normal_values(splits[20], (D, SFF), D ** -0.5, 0.125)
    shared_up = normal_values(splits[21], (D, SFF), D ** -0.5, 0.125)
    shared_down = normal_values(splits[22], (SFF, D), SFF ** -0.5, 0.375)
    second_gain = jnp.clip(1.0 + 0.18 * jax.random.normal(splits[23], (D,), jnp.float32), 0.1, 1.9)
    return dict(stream=stream, conv_cache=conv_cache, scan_state=scan_state, gate_weight=gate_weight, value_weight=value_weight, entry_weight=entry_weight, readout_weight=readout_weight, step_weight=step_weight, conv_weight=conv_weight, step_bias=step_bias, decay_rate=decay_rate, skip_gain=skip_gain, group_gain=group_gain, out_weight=out_weight, first_gain=first_gain, routes=routes, route_weight=route_weight, expert_gate=expert_gate, expert_up=expert_up, expert_down=expert_down, shared_gate=shared_gate, shared_up=shared_up, shared_down=shared_down, second_gain=second_gain)


RESIDUAL_SCALE = 2.0 ** 0.25
NORM_EPSILON = 1e-05
GATED_EPSILON = 1e-06

def rounded(value):
    return lax.optimization_barrier(value.astype(jnp.bfloat16))

def scaled_norm(residual, gain):
    full_width = residual.shape[-1]
    mean_value = lax.optimization_barrier(jnp.sum(residual, axis=-1, keepdims=True)) / full_width
    variance = lax.optimization_barrier(jnp.sum(residual * residual, axis=-1, keepdims=True)) / full_width - mean_value * mean_value
    return (residual - mean_value) * lax.rsqrt(variance + NORM_EPSILON) * gain

def swiglu(inputs, gate_matrix, up_matrix, down_matrix):
    hidden = (jax.nn.silu(jnp.dot(inputs, gate_matrix, preferred_element_type=jnp.float32)) * jnp.dot(inputs, up_matrix, preferred_element_type=jnp.float32)).astype(jnp.bfloat16)
    return rounded(jnp.dot(hidden, down_matrix, preferred_element_type=jnp.float32))

def reference(stream, conv_cache, scan_state, gate_weight, value_weight, entry_weight, readout_weight, step_weight, conv_weight, step_bias, decay_rate, skip_gain, group_gain, out_weight, first_gain, routes, route_weight, expert_gate, expert_up, expert_down, shared_gate, shared_up, shared_down, second_gain):
    row_count = stream.shape[0]
    inner_width = HEADS * HEAD_DIM
    per_group = HEADS // GROUPS

    def project(weight):
        return rounded(jnp.dot(stream, weight, preferred_element_type=jnp.float32))
    gate_rows = project(gate_weight)
    fresh = jnp.concatenate([project(value_weight), project(entry_weight), project(readout_weight)], axis=1)
    step_rows = project(step_weight)
    window = jnp.concatenate([conv_cache, fresh[:, None, :]], axis=1)
    active = jax.nn.silu(lax.optimization_barrier(jnp.sum(window.astype(jnp.float32) * conv_weight.astype(jnp.float32)[None], axis=1)))
    head_in = active[:, :inner_width].reshape(row_count, GROUPS, per_group, HEAD_DIM)
    entry_rows = active[:, inner_width:inner_width + GROUPS * STATE].reshape(row_count, GROUPS, 1, 1, STATE)
    readout_rows = active[:, inner_width + GROUPS * STATE:].reshape(row_count, GROUPS, 1, 1, STATE)
    step_size = jax.nn.softplus(step_rows.astype(jnp.float32) + step_bias).reshape(row_count, GROUPS, per_group)
    retained = jnp.exp(-step_size * decay_rate.reshape(GROUPS, per_group))
    old_state = scan_state.reshape(row_count, GROUPS, per_group, HEAD_DIM, STATE)
    new_state = retained[..., None, None] * old_state + (step_size[..., None] * head_in)[..., None] * entry_rows
    head_out = lax.optimization_barrier(jnp.sum(new_state * readout_rows, axis=-1)) + skip_gain.reshape(GROUPS, per_group)[:, :, None] * head_in
    group_width = inner_width // GROUPS
    gated_out = head_out.reshape(row_count, GROUPS, group_width) * jax.nn.silu(gate_rows.astype(jnp.float32)).reshape(row_count, GROUPS, group_width)
    normed = gated_out * lax.rsqrt(lax.optimization_barrier(jnp.mean(gated_out * gated_out, axis=-1, keepdims=True)) + GATED_EPSILON)
    normed = (normed.reshape(row_count, inner_width) * group_gain).astype(jnp.bfloat16)
    mixer_out = rounded(jnp.dot(normed, out_weight, preferred_element_type=jnp.float32))
    first_rows = rounded(scaled_norm(RESIDUAL_SCALE * stream.astype(jnp.float32) + mixer_out.astype(jnp.float32), first_gain))
    expert_count = expert_gate.shape[0]
    matches = routes[:, :, None] == jnp.arange(expert_count, dtype=jnp.int32)[None, None, :]
    weight_of = lax.optimization_barrier(jnp.sum(jnp.where(matches, route_weight[:, :, None], jnp.zeros_like(route_weight)[:, :, None]), axis=1))

    def one_expert(carry, inputs):
        gate_matrix, up_matrix, down_matrix, column = inputs
        expert_out = swiglu(first_rows, gate_matrix, up_matrix, down_matrix)
        return (carry + column[:, None] * expert_out.astype(jnp.float32), None)
    start_sum = jnp.zeros((row_count, first_rows.shape[1]), jnp.float32)
    routed, _ = lax.scan(one_expert, start_sum, (expert_gate, expert_up, expert_down, weight_of.T))
    shared_out = swiglu(first_rows, shared_gate, shared_up, shared_down)
    moe_sum = routed + shared_out.astype(jnp.float32)
    result = scaled_norm(RESIDUAL_SCALE * first_rows.astype(jnp.float32) + moe_sum, second_gain).astype(jnp.bfloat16)
    return (result, window[:, 1:], new_state.reshape(row_count, HEADS, HEAD_DIM, STATE))
```

```python
import functools

import jax
import jax.numpy as jnp
from jax import lax
from jax.experimental import pallas as pl
from jax.experimental.pallas import tpu as pltpu
from jax.sharding import PartitionSpec as P

HEAD_DIM = 64
STATE = 128
GROUPS = 2
CAP = 8


RESIDUAL_SCALE = 2.0**0.25
NORM_EPSILON = 1e-05
GATED_EPSILON = 1e-06


def rounded(value):
    return lax.optimization_barrier(value.astype(jnp.bfloat16))


def finish_norm(residual, row_total, square, full_width, gain):
    mean_value = (row_total / full_width)[:, None]
    variance = (square / full_width)[:, None] - mean_value * mean_value
    return (residual - mean_value) * lax.rsqrt(variance + NORM_EPSILON) * gain


def swiglu(inputs, gate_matrix, up_matrix, down_matrix):
    hidden = (
        jax.nn.silu(jnp.dot(inputs, gate_matrix, preferred_element_type=jnp.float32))
        * jnp.dot(inputs, up_matrix, preferred_element_type=jnp.float32)
    ).astype(jnp.bfloat16)
    return rounded(jnp.dot(hidden, down_matrix, preferred_element_type=jnp.float32))


def on_device(
    stream,
    conv_cache,
    scan_state,
    gate_weight,
    value_weight,
    entry_weight,
    readout_weight,
    step_weight,
    conv_weight,
    step_bias,
    decay_rate,
    skip_gain,
    group_gain,
    out_weight,
    first_gain,
    routes,
    route_weight,
    expert_gate,
    expert_up,
    expert_down,
    shared_gate,
    shared_up,
    shared_down,
    second_gain,
):
    devices = lax.axis_size("ep")
    device_rank = lax.axis_index("ep")
    own_rows = conv_cache.shape[0]
    row_count = stream.shape[0]
    slice_width = stream.shape[1]
    full_width = slice_width * devices
    inner_width = gate_weight.shape[1]
    head_count = step_weight.shape[1]
    per_group = head_count // GROUPS
    group_width = inner_width // GROUPS
    bounds = (inner_width, 2 * inner_width + 2 * GROUPS * STATE)
    weights_in = (gate_weight, value_weight, entry_weight, readout_weight, step_weight)
    summed = rounded(
        lax.psum_scatter(
            jnp.concatenate(
                [
                    jnp.dot(stream, weight, preferred_element_type=jnp.float32)
                    for weight in weights_in
                ],
                axis=1,
            ),
            "ep",
            scatter_dimension=0,
            tiled=True,
        )
    )
    gate_rows = summed[:, : bounds[0]]
    fresh = summed[:, bounds[0] : bounds[1]]
    step_rows = summed[:, bounds[1] :]
    window = jnp.concatenate([conv_cache, fresh[:, None, :]], axis=1)
    active = jax.nn.silu(
        jnp.sum(window.astype(jnp.float32) * conv_weight.astype(jnp.float32)[None], axis=1)
    )
    head_in = active[:, :inner_width].reshape(own_rows, GROUPS, per_group, HEAD_DIM)
    entry_rows = active[:, inner_width : inner_width + GROUPS * STATE].reshape(
        own_rows, GROUPS, 1, 1, STATE
    )
    readout_rows = active[:, inner_width + GROUPS * STATE :].reshape(own_rows, GROUPS, 1, 1, STATE)
    step_size = jax.nn.softplus(step_rows.astype(jnp.float32) + step_bias).reshape(
        own_rows, GROUPS, per_group
    )
    retained = jnp.exp(-step_size * decay_rate.reshape(GROUPS, per_group))
    old_state = scan_state.reshape(own_rows, GROUPS, per_group, HEAD_DIM, STATE)
    new_state = (
        retained[..., None, None] * old_state
        + (step_size[..., None] * head_in)[..., None] * entry_rows
    )
    head_out = (
        jnp.sum(new_state * readout_rows, axis=-1)
        + skip_gain.reshape(GROUPS, per_group)[:, :, None] * head_in
    )
    gated_out = head_out.reshape(own_rows, GROUPS, group_width) * jax.nn.silu(
        gate_rows.astype(jnp.float32)
    ).reshape(own_rows, GROUPS, group_width)
    normed = gated_out * lax.rsqrt(
        jnp.mean(gated_out * gated_out, axis=-1, keepdims=True) + GATED_EPSILON
    )
    normed = (normed.reshape(own_rows, inner_width) * group_gain).astype(jnp.bfloat16)
    mixer_out = rounded(
        jnp.dot(
            lax.all_gather(normed, "ep", axis=0, tiled=True),
            out_weight,
            preferred_element_type=jnp.float32,
        )
    )
    column_start = device_rank * slice_width
    residual = RESIDUAL_SCALE * stream.astype(jnp.float32) + mixer_out.astype(jnp.float32)
    row_total, square = lax.psum(
        (jnp.sum(residual, axis=1), jnp.sum(residual * residual, axis=1)), "ep"
    )
    gain_part = lax.dynamic_slice_in_dim(first_gain, column_start, slice_width, 0)
    first_part = rounded(finish_norm(residual, row_total, square, full_width, gain_part))
    first_rows = lax.all_gather(first_part, "ep", axis=1, tiled=True)
    matches = routes[:, :, None] == jnp.arange(devices, dtype=jnp.int32)[None, None, :]
    member = jnp.sum(matches.astype(jnp.int32), axis=1)
    weight_of = jnp.sum(jnp.where(matches, route_weight[:, :, None], 0.0), axis=1)
    slot_rank = jnp.cumsum(member, axis=0) - member
    slot_ids = jnp.arange(CAP, dtype=jnp.int32)
    mine_member = lax.dynamic_slice_in_dim(member, device_rank, 1, 1)[:, 0]
    mine_slot = lax.dynamic_slice_in_dim(slot_rank, device_rank, 1, 1)[:, 0]
    chosen = (mine_slot[None, :] == slot_ids[:, None]) & (mine_member[None, :] == 1)
    taken_rows = jnp.dot(
        chosen.astype(jnp.bfloat16), first_rows, preferred_element_type=jnp.float32
    ).astype(jnp.bfloat16)
    expert_out = swiglu(taken_rows, expert_gate[0], expert_up[0], expert_down[0])
    arrived = lax.all_to_all(expert_out, "ep", split_axis=1, concat_axis=0, tiled=True)
    spread = jnp.where(
        (slot_rank[:, :, None] == slot_ids[None, None, :]) & (member[:, :, None] == 1),
        weight_of[:, :, None],
        0.0,
    )
    moe_part = jnp.dot(
        spread.reshape(row_count, devices * CAP),
        arrived.astype(jnp.float32),
        precision=lax.Precision.HIGHEST,
    )
    down_part = lax.dynamic_slice_in_dim(shared_down, column_start, slice_width, 1)
    shared_part = swiglu(first_rows, shared_gate, shared_up, down_part)
    moe_part = moe_part + shared_part.astype(jnp.float32)
    residual_two = RESIDUAL_SCALE * first_part.astype(jnp.float32) + moe_part
    total_two, square_two = lax.psum(
        (jnp.sum(residual_two, axis=1), jnp.sum(residual_two * residual_two, axis=1)), "ep"
    )
    result = finish_norm(residual_two, total_two, square_two, full_width, second_gain).astype(
        jnp.bfloat16
    )
    return (result, window[:, 1:], new_state.reshape(own_rows, head_count, HEAD_DIM, STATE))


MESH = pl.DeviceIdType.MESH
LANES = 128
ROWS = 40


def silu(value):
    return value * (1.0 / (1.0 + jnp.exp(-value)))


def iota(shape, dim):
    return lax.broadcasted_iota(jnp.int32, shape, dim)


def fused_kernel(
    sizes,
    stream,
    conv_cache,
    scan_state,
    gate_weight,
    value_weight,
    entry_weight,
    readout_weight,
    step_weight,
    conv_weight,
    step_bias,
    decay_rate,
    skip_gain,
    group_gain,
    out_weight,
    first_gain,
    routes,
    route_weight,
    expert_gate,
    expert_up,
    expert_down,
    shared_gate,
    shared_up,
    shared_down,
    second_gain,
    result_ref,
    conv_ref,
    state_ref,
    x_v,
    cache_v,
    state_v,
    wg_v,
    wv_v,
    we_v,
    wr_v,
    ws_v,
    cw_v,
    sb_v,
    dr_v,
    sk_v,
    gg_v,
    ow_v,
    fg_v,
    rt_v,
    rw_v,
    eg_v,
    eu_v,
    ed_v,
    sg_v,
    su_v,
    sd_v,
    s2_v,
    conv_v,
    stage,
    part_send,
    part_recv,
    x_recv,
    norm_send,
    norm_recv,
    mix_send,
    mix_recv,
    out_send,
    out_recv,
    stat_send,
    stat_recv,
    taps,
    past,
    gains,
    turn,
    wide,
    firsts,
    load_sem,
    store_sem,
    send_sem,
    recv_sem,
):
    n, inner, groups, head_dim = sizes
    tokens = n
    me = lax.axis_index("ep")
    blocks = inner // LANES
    heads_a_row = LANES // head_dim
    heads = inner // head_dim
    full_width = n * LANES
    barrier = pltpu.get_barrier_semaphore()
    for k in range(1, n):
        pl.semaphore_signal(
            barrier, inc=1, device_id={"ep": lax.rem(me + k, n)}, device_id_type=MESH
        )

    moves = (
        (stream, x_v),
        (step_weight, ws_v),
        (gate_weight, wg_v),
        (value_weight, wv_v),
        (entry_weight, we_v),
        (readout_weight, wr_v),
        (conv_cache, cache_v),
        (conv_weight, cw_v),
        (step_bias, sb_v),
        (decay_rate, dr_v),
        (skip_gain, sk_v),
        (group_gain, gg_v),
        (routes, rt_v),
        (route_weight, rw_v),
        (first_gain, fg_v),
        (second_gain, s2_v),
        (scan_state.at[0], state_v),
        (out_weight, ow_v),
        (expert_gate.at[0], eg_v),
        (expert_up.at[0], eu_v),
        (expert_down.at[0], ed_v),
        (shared_gate, sg_v),
        (shared_up, su_v),
        (shared_down.at[:, pl.ds(pl.multiple_of(me * LANES, LANES), LANES)], sd_v),
    )
    loads = {}
    for index, (source, target) in enumerate(moves):
        copy = pltpu.make_async_copy(source, target, load_sem.at[index])
        copy.start()
        loads[index] = copy

    pending = []

    def post(phase, source, target):
        for k in range(1, n):
            peer = lax.rem(me + k, n)
            copy = pltpu.make_async_remote_copy(
                src_ref=source(peer),
                dst_ref=target.at[me],
                send_sem=send_sem.at[phase, k],
                recv_sem=recv_sem.at[phase, n - k],
                device_id={"ep": peer},
                device_id_type=MESH,
            )
            copy.start()
            pending.append(copy)

    def arrive(phase, target, k):
        sender = lax.rem(me + k, n)
        pltpu.make_async_remote_copy(
            src_ref=target.at[sender],
            dst_ref=target.at[sender],
            send_sem=send_sem.at[phase, k],
            recv_sem=recv_sem.at[phase, k],
            device_id={"ep": sender},
            device_id_type=MESH,
        ).wait_recv()
        return sender

    for index in range(2):
        loads[index].wait()
    x = x_v[...]
    place = (iota((heads, LANES), 0) == iota((heads, LANES), 1)).astype(jnp.bfloat16)
    step_wide = jnp.dot(ws_v[...], place, preferred_element_type=jnp.float32).astype(jnp.bfloat16)
    base = 2 * blocks + 2 * groups
    stage[pl.ds(base, tokens, stride=ROWS), :] = jnp.dot(
        x, step_wide, preferred_element_type=jnp.float32
    )
    for extra in range(base + 1, ROWS):
        stage[pl.ds(extra, tokens, stride=ROWS), :] = jnp.zeros((tokens, LANES), jnp.float32)
    base = 0
    for index, ref in ((2, wg_v), (3, wv_v), (4, we_v), (5, wr_v)):
        loads[index].wait()
        product = jnp.dot(x, ref[...], preferred_element_type=jnp.float32)
        for j in range(ref.shape[1] // LANES):
            stage[pl.ds(base + j, tokens, stride=ROWS), :] = product[
                :, j * LANES : (j + 1) * LANES
            ]
        base += ref.shape[1] // LANES
    for t in range(tokens):
        part_send[t] = stage[t * ROWS : (t + 1) * ROWS, :].astype(jnp.bfloat16)
    pl.semaphore_wait(barrier, n - 1)
    post(0, lambda peer: part_send.at[peer], part_recv)
    post(1, lambda peer: x_v, x_recv)

    for index in range(6, 16):
        loads[index].wait()
    old_rows = cache_v[0].astype(jnp.float32)
    tap_rows = cw_v[...].astype(jnp.float32)
    conv_blocks = tap_rows.shape[1] // LANES
    tap_count = tap_rows.shape[0]
    for j in range(conv_blocks):
        cut = slice(j * LANES, (j + 1) * LANES)
        taps[pl.ds(j, tap_count, stride=24), :] = tap_rows[:, cut]
        past[pl.ds(j, tap_count - 1, stride=24), :] = old_rows[:, cut]
    for j in range(blocks):
        gains[j : j + 1, :] = gg_v[:, j * LANES : (j + 1) * LANES]
    own_row = iota((blocks, heads), 1) // heads_a_row == iota((blocks, heads), 0)
    own_lane = (
        iota((heads, LANES), 0) % heads_a_row == iota((heads, LANES), 1) // head_dim
    ).astype(jnp.float32)

    def expand(row):
        return jnp.dot(
            jnp.where(own_row, jnp.broadcast_to(row, (blocks, heads)), 0.0),
            own_lane,
            precision=lax.Precision.HIGHEST,
            preferred_element_type=jnp.float32,
        )

    bias_rows = expand(sb_v[...])
    decay_rows = expand(dr_v[...])
    skip_rows = expand(sk_v[...])
    before = jnp.zeros((24, LANES), jnp.float32)
    for tap in range(tap_count - 1):
        before = before + past[tap * 24 : (tap + 1) * 24, :] * taps[tap * 24 : (tap + 1) * 24, :]
    last_tap = taps[(tap_count - 1) * 24 : tap_count * 24, :]
    loads[16].wait()

    total = stage[pl.ds(pl.multiple_of(me * ROWS, ROWS), ROWS), :]
    for k in range(1, n):
        sender = arrive(0, part_recv, k)
        total = total + part_recv[sender].astype(jnp.float32)
    total = total.astype(jnp.bfloat16).astype(jnp.float32)
    fresh = total[blocks : blocks + 24, :]
    active = silu(before + fresh * last_tap)
    head_in = active[:blocks, :]
    step_row = total[2 * blocks + 2 * groups : 2 * blocks + 2 * groups + 1, :heads]
    biased = expand(step_row) + bias_rows
    step = jnp.maximum(biased, 0.0) + jnp.log1p(jnp.exp(-jnp.abs(biased)))
    retained = jnp.exp(-step * decay_rows)
    scaled_in = step * head_in
    rows_a_group = blocks // groups
    group_row = iota((blocks, 1), 0) // rows_a_group
    entry = [active[blocks + g : blocks + g + 1, :] for g in range(groups)]
    readout = [active[blocks + groups + g : blocks + groups + g + 1, :] for g in range(groups)]
    lane = iota((LANES, LANES), 1)
    columns = jnp.zeros((LANES, LANES), jnp.float32)
    for r in range(blocks):
        old = state_v[r * heads_a_row : (r + 1) * heads_a_row].reshape(LANES, LANES)
        dots = jnp.sum(old * readout[r // rows_a_group], axis=1, keepdims=True)
        columns = jnp.where(lane == r, dots, columns)
    old_out = columns.T[:blocks, :]
    cross = jnp.zeros((blocks, 1), jnp.float32)
    for g in range(groups):
        both = jnp.sum(entry[g] * readout[g], axis=1, keepdims=True)
        cross = jnp.where(group_row == g, both, cross)
    head_out = retained * old_out + scaled_in * cross + skip_rows * head_in
    gated = head_out * silu(total[:blocks, :])
    squares = jnp.sum(gated * gated, axis=1, keepdims=True)
    inverse = jnp.zeros((blocks, 1), jnp.float32)
    for g in range(groups):
        square = jnp.sum(
            jnp.where(group_row == g, squares, 0.0), axis=0, keepdims=True
        ) / (rows_a_group * LANES)
        inverse = jnp.where(group_row == g, lax.rsqrt(square + GATED_EPSILON), inverse)
    normed = (gated * inverse * gains[...]).astype(jnp.bfloat16)
    norm_send[...] = normed
    post(2, lambda peer: norm_send, norm_recv)
    norm_recv[me] = normed

    turn[0:blocks, :] = scaled_in
    turn[blocks : 2 * blocks, :] = retained
    turn[2 * blocks :, :] = jnp.zeros((LANES - 2 * blocks, LANES), jnp.float32)
    turned = turn[...].T
    for r in range(blocks):
        own = slice(r * heads_a_row, (r + 1) * heads_a_row)
        old = state_v[own].reshape(LANES, LANES)
        new = (
            turned[:, blocks + r : blocks + r + 1] * old
            + turned[:, r : r + 1] * entry[r // rows_a_group]
        )
        state_v[own] = new.reshape(heads_a_row, head_dim, LANES)
    state_out = pltpu.make_async_copy(state_v, state_ref.at[0], store_sem.at[0])
    state_out.start()
    new_row = jnp.concatenate([fresh[j : j + 1, :] for j in range(conv_blocks)], axis=1)
    conv_v[0] = jnp.concatenate([old_rows[1:, :], new_row], axis=0).astype(jnp.bfloat16)
    conv_out = pltpu.make_async_copy(conv_v, conv_ref, store_sem.at[1])
    conv_out.start()
    for index in range(17, len(moves)):
        loads[index].wait()
    x_recv[me] = x
    for k in range(1, n):
        arrive(1, x_recv, k)

    for k in range(1, n):
        arrive(2, norm_recv, k)
    for t in range(tokens):
        wide[t * blocks : (t + 1) * blocks, :] = norm_recv[t].astype(jnp.float32)
    every = jnp.concatenate(
        [wide[pl.ds(r, tokens, stride=blocks), :].astype(jnp.bfloat16) for r in range(blocks)],
        axis=1,
    )
    mixed = jnp.dot(every, ow_v[...], preferred_element_type=jnp.float32).astype(jnp.bfloat16)
    mix_send[...] = mixed
    post(3, lambda peer: mix_send, mix_recv)
    mix_recv[me] = mixed
    mine = jnp.sum(jnp.where(rt_v[...] == me, rw_v[...], 0.0), axis=1, keepdims=True)
    for k in range(1, n):
        arrive(3, mix_recv, k)

    residuals = [
        RESIDUAL_SCALE * x_recv[d].astype(jnp.float32) + mix_recv[d].astype(jnp.float32)
        for d in range(n)
    ]
    sums = residuals[0]
    squares = residuals[0] * residuals[0]
    for d in range(1, n):
        sums = sums + residuals[d]
        squares = squares + residuals[d] * residuals[d]
    mean_value = jnp.sum(sums, axis=1, keepdims=True) / full_width
    variance = jnp.sum(squares, axis=1, keepdims=True) / full_width - mean_value * mean_value
    factor = lax.rsqrt(variance + NORM_EPSILON)
    parts = []
    for d in range(n):
        part = (
            (residuals[d] - mean_value) * factor * fg_v[:, d * LANES : (d + 1) * LANES]
        ).astype(jnp.bfloat16)
        firsts[d] = part
        parts.append(part)
    first_rows = jnp.concatenate(parts, axis=1)

    def hidden(gate_ref, up_ref):
        gate = jnp.dot(first_rows, gate_ref[...], preferred_element_type=jnp.float32)
        up = jnp.dot(first_rows, up_ref[...], preferred_element_type=jnp.float32)
        return (silu(gate) * up).astype(jnp.bfloat16)

    routed = jnp.dot(hidden(eg_v, eu_v), ed_v[...], preferred_element_type=jnp.float32)
    routed = (routed * mine).astype(jnp.bfloat16)
    for d in range(n):
        out_send[d] = routed[:, d * LANES : (d + 1) * LANES]
    post(4, lambda peer: out_send.at[peer], out_recv)
    shared = jnp.dot(hidden(sg_v, su_v), sd_v[...], preferred_element_type=jnp.float32)
    shared = shared.astype(jnp.bfloat16).astype(jnp.float32)
    moe = shared + out_send[me].astype(jnp.float32)
    for k in range(1, n):
        sender = arrive(4, out_recv, k)
        moe = moe + out_recv[sender].astype(jnp.float32)
    residual = RESIDUAL_SCALE * firsts[me].astype(jnp.float32) + moe

    row_total = jnp.sum(residual, axis=1, keepdims=True)
    row_square = jnp.sum(residual * residual, axis=1, keepdims=True)
    token = iota((tokens, LANES), 0)
    place = iota((tokens, LANES), 1)
    compact = jnp.sum(
        jnp.where(place == token, row_total, 0.0)
        + jnp.where(place == token + tokens, row_square, 0.0),
        axis=0,
        keepdims=True,
    )
    stat_send[...] = compact
    post(5, lambda peer: stat_send, stat_recv)
    for k in range(1, n):
        sender = arrive(5, stat_recv, k)
        compact = compact + stat_recv[sender]
    row_total = jnp.sum(jnp.where(place == token, compact, 0.0), axis=1, keepdims=True)
    row_square = jnp.sum(jnp.where(place == token + tokens, compact, 0.0), axis=1, keepdims=True)
    mean_value = row_total / full_width
    variance = row_square / full_width - mean_value * mean_value
    result_ref[...] = (
        (residual - mean_value) * lax.rsqrt(variance + NORM_EPSILON) * s2_v[...]
    ).astype(jnp.bfloat16)
    for copy in pending:
        copy.wait_send()
    state_out.wait()
    conv_out.wait()


def fused(*arrays):
    (stream, conv_cache, scan_state) = arrays[:3]
    n = lax.axis_size("ep")
    inner = arrays[3].shape[1]
    groups = arrays[5].shape[1] // scan_state.shape[3]
    blocks = inner // LANES
    arrays = [a.reshape(1, -1) if a.ndim == 1 else a for a in arrays]
    tile = (stream.shape[0], LANES)
    landing = []
    for index, a in enumerate(arrays):
        shape = a.shape
        if index in (2, 17, 18, 19):
            shape = shape[1:]
        if index == 22:
            shape = (shape[0], LANES)
        landing.append(pltpu.VMEM(shape, a.dtype))
    bf16, f32 = jnp.bfloat16, jnp.float32
    return pl.pallas_call(
        functools.partial(fused_kernel, (n, inner, groups, scan_state.shape[2])),
        out_shape=(
            jax.ShapeDtypeStruct(stream.shape, bf16),
            jax.ShapeDtypeStruct(conv_cache.shape, bf16),
            jax.ShapeDtypeStruct(scan_state.shape, f32),
        ),
        in_specs=[pl.BlockSpec(memory_space=pl.ANY)] * len(arrays),
        out_specs=(
            pl.BlockSpec(memory_space=pltpu.VMEM),
            pl.BlockSpec(memory_space=pl.ANY),
            pl.BlockSpec(memory_space=pl.ANY),
        ),
        scratch_shapes=landing
        + [
            pltpu.VMEM(conv_cache.shape, bf16),
            pltpu.VMEM((n * ROWS, LANES), f32),
            pltpu.VMEM((n, ROWS, LANES), bf16),
            pltpu.VMEM((n, ROWS, LANES), bf16),
            pltpu.VMEM((n,) + tile, bf16),
            pltpu.VMEM((blocks, LANES), bf16),
            pltpu.VMEM((n, blocks, LANES), bf16),
            pltpu.VMEM(tile, bf16),
            pltpu.VMEM((n,) + tile, bf16),
            pltpu.VMEM((n,) + tile, bf16),
            pltpu.VMEM((n,) + tile, bf16),
            pltpu.VMEM((1, LANES), f32),
            pltpu.VMEM((n, 1, LANES), f32),
            pltpu.VMEM((4 * 24, LANES), f32),
            pltpu.VMEM((3 * 24, LANES), f32),
            pltpu.VMEM((blocks, LANES), f32),
            pltpu.VMEM((LANES, LANES), f32),
            pltpu.VMEM((n * blocks, LANES), f32),
            pltpu.VMEM((n,) + tile, bf16),
            pltpu.SemaphoreType.DMA((len(arrays),)),
            pltpu.SemaphoreType.DMA((2,)),
            pltpu.SemaphoreType.DMA((6, n)),
            pltpu.SemaphoreType.DMA((6, n)),
        ],
        compiler_params=pltpu.CompilerParams(
            collective_id=0, has_side_effects=True, vmem_limit_bytes=40 * 1024 * 1024
        ),
    )(*arrays)


def fits(arrays):
    n = lax.axis_size("ep")
    stream, conv_cache, scan_state = arrays[:3]
    head_count, head_dim, state = scan_state.shape[1:]
    blocks = arrays[3].shape[1] // LANES
    groups = arrays[5].shape[1] // LANES
    return (
        stream.shape == (n, LANES)
        and conv_cache.shape[0] == 1
        and state == LANES
        and LANES % head_dim == 0
        and head_count <= LANES
        and blocks % 8 == 0
        and 2 * blocks <= LANES
        and 2 * tokens_of(stream) <= LANES
        and blocks % groups == 0
        and arrays[8].shape[0] == 4
        and blocks + 2 * groups < 24
        and 2 * blocks + 2 * groups < ROWS
    )


def tokens_of(stream):
    return stream.shape[0]


def dispatch(*arrays):
    if fits(arrays):
        return fused(*arrays)
    return on_device(*arrays)


def solution(mesh):
    return jax.shard_map(
        dispatch,
        mesh=mesh,
        in_specs=(
            P("grp", "ep"),
            P(("grp", "ep"), None, None),
            P(("grp", "ep"), None, None, None),
            P("ep", None),
            P("ep", None),
            P("ep", None),
            P("ep", None),
            P("ep", None),
            P(),
            P(),
            P(),
            P(),
            P(),
            P(None, "ep"),
            P(),
            P("grp", None),
            P("grp", None),
            P("ep", None, None),
            P("ep", None, None),
            P("ep", None, None),
            P(),
            P(),
            P(),
            P("ep"),
        ),
        out_specs=(
            P("grp", "ep"),
            P(("grp", "ep"), None, None),
            P(("grp", "ep"), None, None, None),
        ),
        check_vma=False,
    )
```

```python
import functools

import jax
import jax.numpy as jnp
from jax import lax
from jax.experimental import pallas as pl
from jax.experimental.pallas import tpu as pltpu
from jax.sharding import PartitionSpec as P

HEAD_DIM = 64
STATE = 128
GROUPS = 2
CAP = 8


RESIDUAL_SCALE = 2.0**0.25
NORM_EPSILON = 1e-05
GATED_EPSILON = 1e-06


def rounded(value):
    return lax.optimization_barrier(value.astype(jnp.bfloat16))


def finish_norm(residual, row_total, square, full_width, gain):
    mean_value = (row_total / full_width)[:, None]
    variance = (square / full_width)[:, None] - mean_value * mean_value
    return (residual - mean_value) * lax.rsqrt(variance + NORM_EPSILON) * gain


def swiglu(inputs, gate_matrix, up_matrix, down_matrix):
    hidden = (
        jax.nn.silu(jnp.dot(inputs, gate_matrix, preferred_element_type=jnp.float32))
        * jnp.dot(inputs, up_matrix, preferred_element_type=jnp.float32)
    ).astype(jnp.bfloat16)
    return rounded(jnp.dot(hidden, down_matrix, preferred_element_type=jnp.float32))


def on_device(
    stream,
    conv_cache,
    scan_state,
    gate_weight,
    value_weight,
    entry_weight,
    readout_weight,
    step_weight,
    conv_weight,
    step_bias,
    decay_rate,
    skip_gain,
    group_gain,
    out_weight,
    first_gain,
    routes,
    route_weight,
    expert_gate,
    expert_up,
    expert_down,
    shared_gate,
    shared_up,
    shared_down,
    second_gain,
):
    devices = lax.axis_size("ep")
    device_rank = lax.axis_index("ep")
    own_rows = conv_cache.shape[0]
    row_count = stream.shape[0]
    slice_width = stream.shape[1]
    full_width = slice_width * devices
    inner_width = gate_weight.shape[1]
    head_count = step_weight.shape[1]
    per_group = head_count // GROUPS
    group_width = inner_width // GROUPS
    bounds = (inner_width, 2 * inner_width + 2 * GROUPS * STATE)
    weights_in = (gate_weight, value_weight, entry_weight, readout_weight, step_weight)
    summed = rounded(
        lax.psum_scatter(
            jnp.concatenate(
                [
                    jnp.dot(stream, weight, preferred_element_type=jnp.float32)
                    for weight in weights_in
                ],
                axis=1,
            ),
            "ep",
            scatter_dimension=0,
            tiled=True,
        )
    )
    gate_rows = summed[:, : bounds[0]]
    fresh = summed[:, bounds[0] : bounds[1]]
    step_rows = summed[:, bounds[1] :]
    window = jnp.concatenate([conv_cache, fresh[:, None, :]], axis=1)
    active = jax.nn.silu(
        jnp.sum(window.astype(jnp.float32) * conv_weight.astype(jnp.float32)[None], axis=1)
    )
    head_in = active[:, :inner_width].reshape(own_rows, GROUPS, per_group, HEAD_DIM)
    entry_rows = active[:, inner_width : inner_width + GROUPS * STATE].reshape(
        own_rows, GROUPS, 1, 1, STATE
    )
    readout_rows = active[:, inner_width + GROUPS * STATE :].reshape(own_rows, GROUPS, 1, 1, STATE)
    step_size = jax.nn.softplus(step_rows.astype(jnp.float32) + step_bias).reshape(
        own_rows, GROUPS, per_group
    )
    retained = jnp.exp(-step_size * decay_rate.reshape(GROUPS, per_group))
    old_state = scan_state.reshape(own_rows, GROUPS, per_group, HEAD_DIM, STATE)
    new_state = (
        retained[..., None, None] * old_state
        + (step_size[..., None] * head_in)[..., None] * entry_rows
    )
    head_out = (
        jnp.sum(new_state * readout_rows, axis=-1)
        + skip_gain.reshape(GROUPS, per_group)[:, :, None] * head_in
    )
    gated_out = head_out.reshape(own_rows, GROUPS, group_width) * jax.nn.silu(
        gate_rows.astype(jnp.float32)
    ).reshape(own_rows, GROUPS, group_width)
    normed = gated_out * lax.rsqrt(
        jnp.mean(gated_out * gated_out, axis=-1, keepdims=True) + GATED_EPSILON
    )
    normed = (normed.reshape(own_rows, inner_width) * group_gain).astype(jnp.bfloat16)
    mixer_out = rounded(
        jnp.dot(
            lax.all_gather(normed, "ep", axis=0, tiled=True),
            out_weight,
            preferred_element_type=jnp.float32,
        )
    )
    column_start = device_rank * slice_width
    residual = RESIDUAL_SCALE * stream.astype(jnp.float32) + mixer_out.astype(jnp.float32)
    row_total, square = lax.psum(
        (jnp.sum(residual, axis=1), jnp.sum(residual * residual, axis=1)), "ep"
    )
    gain_part = lax.dynamic_slice_in_dim(first_gain, column_start, slice_width, 0)
    first_part = rounded(finish_norm(residual, row_total, square, full_width, gain_part))
    first_rows = lax.all_gather(first_part, "ep", axis=1, tiled=True)
    matches = routes[:, :, None] == jnp.arange(devices, dtype=jnp.int32)[None, None, :]
    member = jnp.sum(matches.astype(jnp.int32), axis=1)
    weight_of = jnp.sum(jnp.where(matches, route_weight[:, :, None], 0.0), axis=1)
    slot_rank = jnp.cumsum(member, axis=0) - member
    slot_ids = jnp.arange(CAP, dtype=jnp.int32)
    mine_member = lax.dynamic_slice_in_dim(member, device_rank, 1, 1)[:, 0]
    mine_slot = lax.dynamic_slice_in_dim(slot_rank, device_rank, 1, 1)[:, 0]
    chosen = (mine_slot[None, :] == slot_ids[:, None]) & (mine_member[None, :] == 1)
    taken_rows = jnp.dot(
        chosen.astype(jnp.bfloat16), first_rows, preferred_element_type=jnp.float32
    ).astype(jnp.bfloat16)
    expert_out = swiglu(taken_rows, expert_gate[0], expert_up[0], expert_down[0])
    arrived = lax.all_to_all(expert_out, "ep", split_axis=1, concat_axis=0, tiled=True)
    spread = jnp.where(
        (slot_rank[:, :, None] == slot_ids[None, None, :]) & (member[:, :, None] == 1),
        weight_of[:, :, None],
        0.0,
    )
    moe_part = jnp.dot(
        spread.reshape(row_count, devices * CAP),
        arrived.astype(jnp.float32),
        precision=lax.Precision.HIGHEST,
    )
    down_part = lax.dynamic_slice_in_dim(shared_down, column_start, slice_width, 1)
    shared_part = swiglu(first_rows, shared_gate, shared_up, down_part)
    moe_part = moe_part + shared_part.astype(jnp.float32)
    residual_two = RESIDUAL_SCALE * first_part.astype(jnp.float32) + moe_part
    total_two, square_two = lax.psum(
        (jnp.sum(residual_two, axis=1), jnp.sum(residual_two * residual_two, axis=1)), "ep"
    )
    result = finish_norm(residual_two, total_two, square_two, full_width, second_gain).astype(
        jnp.bfloat16
    )
    return (result, window[:, 1:], new_state.reshape(own_rows, head_count, HEAD_DIM, STATE))


MESH = pl.DeviceIdType.MESH
LANES = 128
ROWS = 40


def silu(value):
    return value * (1.0 / (1.0 + jnp.exp(-value)))


def iota(shape, dim):
    return lax.broadcasted_iota(jnp.int32, shape, dim)


def fused_kernel(
    sizes,
    stream,
    conv_cache,
    scan_state,
    gate_weight,
    value_weight,
    entry_weight,
    readout_weight,
    step_weight,
    conv_weight,
    step_bias,
    decay_rate,
    skip_gain,
    group_gain,
    out_weight,
    first_gain,
    routes,
    route_weight,
    expert_gate,
    expert_up,
    expert_down,
    shared_gate,
    shared_up,
    shared_down,
    second_gain,
    result_ref,
    conv_ref,
    state_ref,
    x_v,
    cache_v,
    state_v,
    wg_v,
    wv_v,
    we_v,
    wr_v,
    ws_v,
    cw_v,
    sb_v,
    dr_v,
    sk_v,
    gg_v,
    ow_v,
    fg_v,
    rt_v,
    rw_v,
    eg_v,
    eu_v,
    ed_v,
    sg_v,
    su_v,
    sd_v,
    s2_v,
    conv_v,
    stage,
    part_recv,
    x_recv,
    norm_send,
    norm_recv,
    mix_send,
    mix_recv,
    out_send,
    out_recv,
    stat_send,
    stat_recv,
    taps,
    past,
    gains,
    turn,
    wide,
    firsts,
    load_sem,
    store_sem,
    send_sem,
    recv_sem,
):
    n, inner, groups, head_dim = sizes
    tokens = n
    me = lax.axis_index("ep")
    blocks = inner // LANES
    heads_a_row = LANES // head_dim
    heads = inner // head_dim
    full_width = n * LANES
    barrier = pltpu.get_barrier_semaphore()
    for k in range(1, n):
        pl.semaphore_signal(
            barrier, inc=1, device_id={"ep": lax.rem(me + k, n)}, device_id_type=MESH
        )

    moves = (
        (stream, x_v),
        (step_weight, ws_v),
        (gate_weight, wg_v),
        (value_weight, wv_v),
        (entry_weight, we_v),
        (readout_weight, wr_v),
        (conv_cache, cache_v),
        (conv_weight, cw_v),
        (step_bias, sb_v),
        (decay_rate, dr_v),
        (skip_gain, sk_v),
        (group_gain, gg_v),
        (routes, rt_v),
        (route_weight, rw_v),
        (first_gain, fg_v),
        (second_gain, s2_v),
        (scan_state.at[0], state_v),
        (out_weight, ow_v),
        (expert_gate.at[0], eg_v),
        (expert_up.at[0], eu_v),
        (expert_down.at[0], ed_v),
        (shared_gate, sg_v),
        (shared_up, su_v),
        (shared_down.at[:, pl.ds(pl.multiple_of(me * LANES, LANES), LANES)], sd_v),
    )
    loads = {}
    for index, (source, target) in enumerate(moves):
        copy = pltpu.make_async_copy(source, target, load_sem.at[index])
        copy.start()
        loads[index] = copy

    pending = []

    def post(phase, source, target):
        for k in range(1, n):
            peer = lax.rem(me + k, n)
            copy = pltpu.make_async_remote_copy(
                src_ref=source(peer),
                dst_ref=target.at[me],
                send_sem=send_sem.at[phase, k],
                recv_sem=recv_sem.at[phase, n - k],
                device_id={"ep": peer},
                device_id_type=MESH,
            )
            copy.start()
            pending.append(copy)

    def arrive(phase, target, k):
        sender = lax.rem(me + k, n)
        pltpu.make_async_remote_copy(
            src_ref=target.at[sender],
            dst_ref=target.at[sender],
            send_sem=send_sem.at[phase, k],
            recv_sem=recv_sem.at[phase, k],
            device_id={"ep": sender},
            device_id_type=MESH,
        ).wait_recv()
        return sender

    for index in range(2):
        loads[index].wait()
    x = x_v[...]
    place = (iota((heads, LANES), 0) == iota((heads, LANES), 1)).astype(jnp.bfloat16)
    step_wide = lax.dot_general(
        place, ws_v[...], (((0,), (0,)), ((), ())), preferred_element_type=jnp.float32
    ).astype(jnp.bfloat16)
    base = 2 * blocks + 2 * groups
    stage[pl.ds(base, tokens, stride=ROWS), :] = lax.dot_general(
        x, step_wide, (((1,), (1,)), ((), ())), preferred_element_type=jnp.float32
    )
    for extra in range(base + 1, ROWS):
        stage[pl.ds(extra, tokens, stride=ROWS), :] = jnp.zeros((tokens, LANES), jnp.float32)
    base = 0
    for index, ref in ((2, wg_v), (3, wv_v), (4, we_v), (5, wr_v)):
        loads[index].wait()
        product = jnp.dot(x, ref[...], preferred_element_type=jnp.float32)
        for j in range(ref.shape[1] // LANES):
            stage[pl.ds(base + j, tokens, stride=ROWS), :] = product[
                :, j * LANES : (j + 1) * LANES
            ]
        base += ref.shape[1] // LANES
    pl.semaphore_wait(barrier, n - 1)
    post(0, lambda peer: stage.at[pl.ds(pl.multiple_of(peer * ROWS, ROWS), ROWS)], part_recv)

    for index in range(6, 16):
        loads[index].wait()
    old_rows = cache_v[0].astype(jnp.float32)
    tap_rows = cw_v[...].astype(jnp.float32)
    conv_blocks = tap_rows.shape[1] // LANES
    tap_count = tap_rows.shape[0]
    for j in range(conv_blocks):
        cut = slice(j * LANES, (j + 1) * LANES)
        taps[pl.ds(j, tap_count, stride=24), :] = tap_rows[:, cut]
        past[pl.ds(j, tap_count - 1, stride=24), :] = old_rows[:, cut]
    for j in range(blocks):
        gains[j : j + 1, :] = gg_v[:, j * LANES : (j + 1) * LANES]
    own_row = iota((blocks, heads), 1) // heads_a_row == iota((blocks, heads), 0)
    own_lane = (
        iota((heads, LANES), 0) % heads_a_row == iota((heads, LANES), 1) // head_dim
    ).astype(jnp.float32)

    def expand(row):
        return jnp.dot(
            jnp.where(own_row, jnp.broadcast_to(row, (blocks, heads)), 0.0),
            own_lane,
            precision=lax.Precision.HIGHEST,
            preferred_element_type=jnp.float32,
        )

    bias_rows = expand(sb_v[...])
    decay_rows = expand(dr_v[...])
    skip_rows = expand(sk_v[...])
    before = jnp.zeros((24, LANES), jnp.float32)
    for tap in range(tap_count - 1):
        before = before + past[tap * 24 : (tap + 1) * 24, :] * taps[tap * 24 : (tap + 1) * 24, :]
    last_tap = taps[(tap_count - 1) * 24 : tap_count * 24, :]
    loads[16].wait()

    total = stage[pl.ds(pl.multiple_of(me * ROWS, ROWS), ROWS), :]
    for k in range(1, n):
        sender = arrive(0, part_recv, k)
        total = total + part_recv[sender]
    post(1, lambda peer: x_v, x_recv)
    total = total.astype(jnp.bfloat16).astype(jnp.float32)
    fresh = total[blocks : blocks + 24, :]
    active = silu(before + fresh * last_tap)
    head_in = active[:blocks, :]
    step_row = total[2 * blocks + 2 * groups : 2 * blocks + 2 * groups + 1, :heads]
    biased = expand(step_row) + bias_rows
    step = jnp.maximum(biased, 0.0) + jnp.log1p(jnp.exp(-jnp.abs(biased)))
    retained = jnp.exp(-step * decay_rows)
    scaled_in = step * head_in
    rows_a_group = blocks // groups
    group_row = iota((blocks, 1), 0) // rows_a_group
    entry = [active[blocks + g : blocks + g + 1, :] for g in range(groups)]
    readout = [active[blocks + groups + g : blocks + groups + g + 1, :] for g in range(groups)]
    lane = iota((LANES, LANES), 1)
    columns = jnp.zeros((LANES, LANES), jnp.float32)
    for r in range(blocks):
        old = state_v[r * heads_a_row : (r + 1) * heads_a_row].reshape(LANES, LANES)
        dots = jnp.sum(old * readout[r // rows_a_group], axis=1, keepdims=True)
        columns = jnp.where(lane == r, dots, columns)
    old_out = columns.T[:blocks, :]
    cross = jnp.zeros((blocks, 1), jnp.float32)
    for g in range(groups):
        both = jnp.sum(entry[g] * readout[g], axis=1, keepdims=True)
        cross = jnp.where(group_row == g, both, cross)
    head_out = retained * old_out + scaled_in * cross + skip_rows * head_in
    gated = head_out * silu(total[:blocks, :])
    squares = jnp.sum(gated * gated, axis=1, keepdims=True)
    inverse = jnp.zeros((blocks, 1), jnp.float32)
    for g in range(groups):
        square = jnp.sum(
            jnp.where(group_row == g, squares, 0.0), axis=0, keepdims=True
        ) / (rows_a_group * LANES)
        inverse = jnp.where(group_row == g, lax.rsqrt(square + GATED_EPSILON), inverse)
    normed = (gated * inverse * gains[...]).astype(jnp.bfloat16)
    norm_send[...] = normed
    post(2, lambda peer: norm_send, norm_recv)
    norm_recv[me] = normed

    turn[0:blocks, :] = scaled_in
    turn[blocks : 2 * blocks, :] = retained
    turn[2 * blocks :, :] = jnp.zeros((LANES - 2 * blocks, LANES), jnp.float32)
    turned = turn[...].T
    for r in range(blocks):
        own = slice(r * heads_a_row, (r + 1) * heads_a_row)
        old = state_v[own].reshape(LANES, LANES)
        new = (
            turned[:, blocks + r : blocks + r + 1] * old
            + turned[:, r : r + 1] * entry[r // rows_a_group]
        )
        state_v[own] = new.reshape(heads_a_row, head_dim, LANES)
    state_out = pltpu.make_async_copy(state_v, state_ref.at[0], store_sem.at[0])
    state_out.start()
    new_row = jnp.concatenate([fresh[j : j + 1, :] for j in range(conv_blocks)], axis=1)
    conv_v[0] = jnp.concatenate([old_rows[1:, :], new_row], axis=0).astype(jnp.bfloat16)
    conv_out = pltpu.make_async_copy(conv_v, conv_ref, store_sem.at[1])
    conv_out.start()
    for index in range(17, len(moves)):
        loads[index].wait()
    x_recv[me] = x
    for k in range(1, n):
        arrive(1, x_recv, k)

    for k in range(1, n):
        arrive(2, norm_recv, k)
    for t in range(tokens):
        wide[t * blocks : (t + 1) * blocks, :] = norm_recv[t].astype(jnp.float32)
    every = jnp.concatenate(
        [wide[pl.ds(r, tokens, stride=blocks), :].astype(jnp.bfloat16) for r in range(blocks)],
        axis=1,
    )
    mixed = jnp.dot(every, ow_v[...], preferred_element_type=jnp.float32).astype(jnp.bfloat16)
    mix_send[...] = mixed
    post(3, lambda peer: mix_send, mix_recv)
    mix_recv[me] = mixed
    mine = jnp.sum(jnp.where(rt_v[...] == me, rw_v[...], 0.0), axis=0, keepdims=True)
    same = iota((tokens, tokens), 0) == iota((tokens, tokens), 1)
    mine = jnp.sum(jnp.where(same, mine, 0.0), axis=1, keepdims=True)
    for k in range(1, n):
        arrive(3, mix_recv, k)

    residuals = [
        RESIDUAL_SCALE * x_recv[d].astype(jnp.float32) + mix_recv[d].astype(jnp.float32)
        for d in range(n)
    ]
    sums = residuals[0]
    squares = residuals[0] * residuals[0]
    for d in range(1, n):
        sums = sums + residuals[d]
        squares = squares + residuals[d] * residuals[d]
    mean_value = jnp.sum(sums, axis=1, keepdims=True) / full_width
    variance = jnp.sum(squares, axis=1, keepdims=True) / full_width - mean_value * mean_value
    factor = lax.rsqrt(variance + NORM_EPSILON)
    parts = []
    for d in range(n):
        part = (
            (residuals[d] - mean_value) * factor * fg_v[:, d * LANES : (d + 1) * LANES]
        ).astype(jnp.bfloat16)
        firsts[d] = part
        parts.append(part)
    first_rows = jnp.concatenate(parts, axis=1)

    def hidden(gate_ref, up_ref):
        gate = jnp.dot(first_rows, gate_ref[...], preferred_element_type=jnp.float32)
        up = jnp.dot(first_rows, up_ref[...], preferred_element_type=jnp.float32)
        return (silu(gate) * up).astype(jnp.bfloat16)

    routed = jnp.dot(hidden(eg_v, eu_v), ed_v[...], preferred_element_type=jnp.float32)
    routed = (routed * mine).astype(jnp.bfloat16)
    for d in range(n):
        out_send[d] = routed[:, d * LANES : (d + 1) * LANES]
    post(4, lambda peer: out_send.at[peer], out_recv)
    shared = jnp.dot(hidden(sg_v, su_v), sd_v[...], preferred_element_type=jnp.float32)
    shared = shared.astype(jnp.bfloat16).astype(jnp.float32)
    moe = shared + out_send[me].astype(jnp.float32)
    for k in range(1, n):
        sender = arrive(4, out_recv, k)
        moe = moe + out_recv[sender].astype(jnp.float32)
    residual = RESIDUAL_SCALE * firsts[me].astype(jnp.float32) + moe

    row_total = jnp.sum(residual, axis=1, keepdims=True)
    row_square = jnp.sum(residual * residual, axis=1, keepdims=True)
    token = iota((tokens, LANES), 0)
    place = iota((tokens, LANES), 1)
    compact = jnp.sum(
        jnp.where(place == token, row_total, 0.0)
        + jnp.where(place == token + tokens, row_square, 0.0),
        axis=0,
        keepdims=True,
    )
    stat_send[...] = compact
    post(5, lambda peer: stat_send, stat_recv)
    for k in range(1, n):
        sender = arrive(5, stat_recv, k)
        compact = compact + stat_recv[sender]
    row_total = jnp.sum(jnp.where(place == token, compact, 0.0), axis=1, keepdims=True)
    row_square = jnp.sum(jnp.where(place == token + tokens, compact, 0.0), axis=1, keepdims=True)
    mean_value = row_total / full_width
    variance = row_square / full_width - mean_value * mean_value
    result_ref[...] = (
        (residual - mean_value) * lax.rsqrt(variance + NORM_EPSILON) * s2_v[...]
    ).astype(jnp.bfloat16)
    for copy in pending:
        copy.wait_send()
    state_out.wait()
    conv_out.wait()


def fused(*arrays):
    (stream, conv_cache, scan_state) = arrays[:3]
    conv_weight = arrays[8]
    n = lax.axis_size("ep")
    inner = arrays[3].shape[1]
    groups = arrays[5].shape[1] // scan_state.shape[3]
    blocks = inner // LANES
    arrays = [a.reshape(1, -1) if a.ndim == 1 else a for a in arrays]
    for index in (7, 15, 16):
        arrays[index] = arrays[index].T
    tile = (stream.shape[0], LANES)
    landing = []
    for index, a in enumerate(arrays):
        shape = a.shape
        if index in (2, 17, 18, 19):
            shape = shape[1:]
        if index == 22:
            shape = (shape[0], LANES)
        landing.append(pltpu.VMEM(shape, a.dtype))
    bf16, f32 = jnp.bfloat16, jnp.float32
    return pl.pallas_call(
        functools.partial(fused_kernel, (n, inner, groups, scan_state.shape[2])),
        out_shape=(
            jax.ShapeDtypeStruct(stream.shape, bf16),
            jax.ShapeDtypeStruct(conv_cache.shape, bf16),
            jax.ShapeDtypeStruct(scan_state.shape, f32),
        ),
        in_specs=[pl.BlockSpec(memory_space=pltpu.HBM)] * len(arrays),
        out_specs=(
            pl.BlockSpec(memory_space=pltpu.VMEM),
            pl.BlockSpec(memory_space=pl.ANY),
            pl.BlockSpec(memory_space=pl.ANY),
        ),
        scratch_shapes=landing
        + [
            pltpu.VMEM(conv_cache.shape, bf16),
            pltpu.VMEM((n * ROWS, LANES), f32),
            pltpu.VMEM((n, ROWS, LANES), f32),
            pltpu.VMEM((n,) + tile, bf16),
            pltpu.VMEM((blocks, LANES), bf16),
            pltpu.VMEM((n, blocks, LANES), bf16),
            pltpu.VMEM(tile, bf16),
            pltpu.VMEM((n,) + tile, bf16),
            pltpu.VMEM((n,) + tile, bf16),
            pltpu.VMEM((n,) + tile, bf16),
            pltpu.VMEM((1, LANES), f32),
            pltpu.VMEM((n, 1, LANES), f32),
            pltpu.VMEM((conv_weight.shape[0] * 24, LANES), f32),
            pltpu.VMEM((conv_cache.shape[1] * 24, LANES), f32),
            pltpu.VMEM((blocks, LANES), f32),
            pltpu.VMEM((LANES, LANES), f32),
            pltpu.VMEM((n * blocks, LANES), f32),
            pltpu.VMEM((n,) + tile, bf16),
            pltpu.SemaphoreType.DMA((len(arrays),)),
            pltpu.SemaphoreType.DMA((2,)),
            pltpu.SemaphoreType.DMA((6, n)),
            pltpu.SemaphoreType.DMA((6, n)),
        ],
        compiler_params=pltpu.CompilerParams(
            collective_id=0, has_side_effects=True, vmem_limit_bytes=67043328
        ),
    )(*arrays)


def fits(arrays):
    n = lax.axis_size("ep")
    stream, conv_cache, scan_state = arrays[:3]
    head_count, head_dim, state = scan_state.shape[1:]
    blocks = arrays[3].shape[1] // LANES
    groups = arrays[5].shape[1] // LANES
    return (
        stream.shape == (n, LANES)
        and conv_cache.shape[0] == 1
        and state == LANES
        and LANES % head_dim == 0
        and head_count <= LANES
        and blocks % 8 == 0
        and 2 * blocks <= LANES
        and 2 * tokens_of(stream) <= LANES
        and blocks % groups == 0
        and arrays[8].shape[0] == conv_cache.shape[1] + 1
        and blocks + 2 * groups < 24
        and 2 * blocks + 2 * groups < ROWS
    )


def tokens_of(stream):
    return stream.shape[0]


def dispatch(*arrays):
    if fits(arrays):
        return fused(*arrays)
    return on_device(*arrays)


def solution(mesh):
    return jax.shard_map(
        dispatch,
        mesh=mesh,
        in_specs=(
            P("grp", "ep"),
            P(("grp", "ep"), None, None),
            P(("grp", "ep"), None, None, None),
            P("ep", None),
            P("ep", None),
            P("ep", None),
            P("ep", None),
            P("ep", None),
            P(),
            P(),
            P(),
            P(),
            P(),
            P(None, "ep"),
            P(),
            P("grp", None),
            P("grp", None),
            P("ep", None, None),
            P("ep", None, None),
            P("ep", None, None),
            P(),
            P(),
            P(),
            P("ep"),
        ),
        out_specs=(
            P("grp", "ep"),
            P(("grp", "ep"), None, None),
            P(("grp", "ep"), None, None, None),
        ),
        check_vma=False,
    )
```

```python
import functools

import jax
import jax.numpy as jnp
from jax import lax
from jax.experimental import pallas as pl
from jax.experimental.pallas import tpu as pltpu
from jax.sharding import PartitionSpec as P

HEAD_DIM = 64
STATE = 128
GROUPS = 2
CAP = 8


RESIDUAL_SCALE = 2.0**0.25
NORM_EPSILON = 1e-05
GATED_EPSILON = 1e-06


def rounded(value):
    return lax.optimization_barrier(value.astype(jnp.bfloat16))


def finish_norm(residual, row_total, square, full_width, gain):
    mean_value = (row_total / full_width)[:, None]
    variance = (square / full_width)[:, None] - mean_value * mean_value
    return (residual - mean_value) * lax.rsqrt(variance + NORM_EPSILON) * gain


def swiglu(inputs, gate_matrix, up_matrix, down_matrix):
    hidden = (
        jax.nn.silu(jnp.dot(inputs, gate_matrix, preferred_element_type=jnp.float32))
        * jnp.dot(inputs, up_matrix, preferred_element_type=jnp.float32)
    ).astype(jnp.bfloat16)
    return rounded(jnp.dot(hidden, down_matrix, preferred_element_type=jnp.float32))


def on_device(
    stream,
    conv_cache,
    scan_state,
    gate_weight,
    value_weight,
    entry_weight,
    readout_weight,
    step_weight,
    conv_weight,
    step_bias,
    decay_rate,
    skip_gain,
    group_gain,
    out_weight,
    first_gain,
    routes,
    route_weight,
    expert_gate,
    expert_up,
    expert_down,
    shared_gate,
    shared_up,
    shared_down,
    second_gain,
):
    devices = lax.axis_size("ep")
    device_rank = lax.axis_index("ep")
    own_rows = conv_cache.shape[0]
    row_count = stream.shape[0]
    slice_width = stream.shape[1]
    full_width = slice_width * devices
    inner_width = gate_weight.shape[1]
    head_count = step_weight.shape[1]
    per_group = head_count // GROUPS
    group_width = inner_width // GROUPS
    bounds = (inner_width, 2 * inner_width + 2 * GROUPS * STATE)
    weights_in = (gate_weight, value_weight, entry_weight, readout_weight, step_weight)
    summed = rounded(
        lax.psum_scatter(
            jnp.concatenate(
                [
                    jnp.dot(stream, weight, preferred_element_type=jnp.float32)
                    for weight in weights_in
                ],
                axis=1,
            ),
            "ep",
            scatter_dimension=0,
            tiled=True,
        )
    )
    gate_rows = summed[:, : bounds[0]]
    fresh = summed[:, bounds[0] : bounds[1]]
    step_rows = summed[:, bounds[1] :]
    window = jnp.concatenate([conv_cache, fresh[:, None, :]], axis=1)
    active = jax.nn.silu(
        jnp.sum(window.astype(jnp.float32) * conv_weight.astype(jnp.float32)[None], axis=1)
    )
    head_in = active[:, :inner_width].reshape(own_rows, GROUPS, per_group, HEAD_DIM)
    entry_rows = active[:, inner_width : inner_width + GROUPS * STATE].reshape(
        own_rows, GROUPS, 1, 1, STATE
    )
    readout_rows = active[:, inner_width + GROUPS * STATE :].reshape(own_rows, GROUPS, 1, 1, STATE)
    step_size = jax.nn.softplus(step_rows.astype(jnp.float32) + step_bias).reshape(
        own_rows, GROUPS, per_group
    )
    retained = jnp.exp(-step_size * decay_rate.reshape(GROUPS, per_group))
    old_state = scan_state.reshape(own_rows, GROUPS, per_group, HEAD_DIM, STATE)
    new_state = (
        retained[..., None, None] * old_state
        + (step_size[..., None] * head_in)[..., None] * entry_rows
    )
    head_out = (
        jnp.sum(new_state * readout_rows, axis=-1)
        + skip_gain.reshape(GROUPS, per_group)[:, :, None] * head_in
    )
    gated_out = head_out.reshape(own_rows, GROUPS, group_width) * jax.nn.silu(
        gate_rows.astype(jnp.float32)
    ).reshape(own_rows, GROUPS, group_width)
    normed = gated_out * lax.rsqrt(
        jnp.mean(gated_out * gated_out, axis=-1, keepdims=True) + GATED_EPSILON
    )
    normed = (normed.reshape(own_rows, inner_width) * group_gain).astype(jnp.bfloat16)
    mixer_out = rounded(
        jnp.dot(
            lax.all_gather(normed, "ep", axis=0, tiled=True),
            out_weight,
            preferred_element_type=jnp.float32,
        )
    )
    column_start = device_rank * slice_width
    residual = RESIDUAL_SCALE * stream.astype(jnp.float32) + mixer_out.astype(jnp.float32)
    row_total, square = lax.psum(
        (jnp.sum(residual, axis=1), jnp.sum(residual * residual, axis=1)), "ep"
    )
    gain_part = lax.dynamic_slice_in_dim(first_gain, column_start, slice_width, 0)
    first_part = rounded(finish_norm(residual, row_total, square, full_width, gain_part))
    first_rows = lax.all_gather(first_part, "ep", axis=1, tiled=True)
    matches = routes[:, :, None] == jnp.arange(devices, dtype=jnp.int32)[None, None, :]
    member = jnp.sum(matches.astype(jnp.int32), axis=1)
    weight_of = jnp.sum(jnp.where(matches, route_weight[:, :, None], 0.0), axis=1)
    slot_rank = jnp.cumsum(member, axis=0) - member
    slot_ids = jnp.arange(CAP, dtype=jnp.int32)
    mine_member = lax.dynamic_slice_in_dim(member, device_rank, 1, 1)[:, 0]
    mine_slot = lax.dynamic_slice_in_dim(slot_rank, device_rank, 1, 1)[:, 0]
    chosen = (mine_slot[None, :] == slot_ids[:, None]) & (mine_member[None, :] == 1)
    taken_rows = jnp.dot(
        chosen.astype(jnp.bfloat16), first_rows, preferred_element_type=jnp.float32
    ).astype(jnp.bfloat16)
    expert_out = swiglu(taken_rows, expert_gate[0], expert_up[0], expert_down[0])
    arrived = lax.all_to_all(expert_out, "ep", split_axis=1, concat_axis=0, tiled=True)
    spread = jnp.where(
        (slot_rank[:, :, None] == slot_ids[None, None, :]) & (member[:, :, None] == 1),
        weight_of[:, :, None],
        0.0,
    )
    moe_part = jnp.dot(
        spread.reshape(row_count, devices * CAP),
        arrived.astype(jnp.float32),
        precision=lax.Precision.HIGHEST,
    )
    down_part = lax.dynamic_slice_in_dim(shared_down, column_start, slice_width, 1)
    shared_part = swiglu(first_rows, shared_gate, shared_up, down_part)
    moe_part = moe_part + shared_part.astype(jnp.float32)
    residual_two = RESIDUAL_SCALE * first_part.astype(jnp.float32) + moe_part
    total_two, square_two = lax.psum(
        (jnp.sum(residual_two, axis=1), jnp.sum(residual_two * residual_two, axis=1)), "ep"
    )
    result = finish_norm(residual_two, total_two, square_two, full_width, second_gain).astype(
        jnp.bfloat16
    )
    return (result, window[:, 1:], new_state.reshape(own_rows, head_count, HEAD_DIM, STATE))


MESH = pl.DeviceIdType.MESH
LANES = 128
ROWS = 40


def silu(value):
    return value * (1.0 / (1.0 + jnp.exp(-value)))


def iota(shape, dim):
    return lax.broadcasted_iota(jnp.int32, shape, dim)


def fused_kernel(
    sizes,
    stream,
    conv_cache,
    scan_state,
    gate_weight,
    value_weight,
    entry_weight,
    readout_weight,
    step_weight,
    conv_weight,
    step_bias,
    decay_rate,
    skip_gain,
    group_gain,
    out_weight,
    first_gain,
    routes,
    route_weight,
    expert_gate,
    expert_up,
    expert_down,
    shared_gate,
    shared_up,
    shared_down,
    second_gain,
    result_ref,
    conv_ref,
    state_ref,
    x_v,
    cache_v,
    state_v,
    wg_v,
    wv_v,
    we_v,
    wr_v,
    ws_v,
    cw_v,
    sb_v,
    dr_v,
    sk_v,
    gg_v,
    ow_v,
    fg_v,
    rt_v,
    rw_v,
    eg_v,
    eu_v,
    ed_v,
    sg_v,
    su_v,
    sd_v,
    s2_v,
    conv_v,
    stage,
    pair_recv,
    part_recv,
    x_recv,
    norm_send,
    norm_recv,
    mix_send,
    mix_recv,
    out_send,
    out_recv,
    stat_send,
    stat_recv,
    taps,
    past,
    gains,
    turn,
    wide,
    firsts,
    load_sem,
    store_sem,
    send_sem,
    recv_sem,
):
    n, inner, groups, head_dim = sizes
    tokens = n
    me = lax.axis_index("ep")
    blocks = inner // LANES
    heads_a_row = LANES // head_dim
    heads = inner // head_dim
    full_width = n * LANES
    barrier = pltpu.get_barrier_semaphore()
    for k in range(1, n):
        pl.semaphore_signal(
            barrier, inc=1, device_id={"ep": lax.rem(me + k, n)}, device_id_type=MESH
        )

    moves = (
        (stream, x_v),
        (step_weight, ws_v),
        (gate_weight, wg_v),
        (value_weight, wv_v),
        (entry_weight, we_v),
        (readout_weight, wr_v),
        (conv_cache, cache_v),
        (conv_weight, cw_v),
        (step_bias, sb_v),
        (decay_rate, dr_v),
        (skip_gain, sk_v),
        (group_gain, gg_v),
        (routes, rt_v),
        (route_weight, rw_v),
        (first_gain, fg_v),
        (second_gain, s2_v),
        (scan_state.at[0], state_v),
        (out_weight, ow_v),
        (expert_gate.at[0], eg_v),
        (expert_up.at[0], eu_v),
        (expert_down.at[0], ed_v),
        (shared_gate, sg_v),
        (shared_up, su_v),
        (shared_down.at[:, pl.ds(pl.multiple_of(me * LANES, LANES), LANES)], sd_v),
    )
    loads = {}
    for index, (source, target) in enumerate(moves):
        copy = pltpu.make_async_copy(source, target, load_sem.at[index])
        copy.start()
        loads[index] = copy

    pending = []

    def post(phase, source, target, stride=1):
        for k in range(stride, n, stride):
            peer = lax.rem(me + k, n)
            copy = pltpu.make_async_remote_copy(
                src_ref=source(peer),
                dst_ref=target.at[me],
                send_sem=send_sem.at[phase, k],
                recv_sem=recv_sem.at[phase, n - k],
                device_id={"ep": peer},
                device_id_type=MESH,
            )
            copy.start()
            pending.append(copy)

    def arrive(phase, target, k):
        sender = lax.rem(me + k, n)
        pltpu.make_async_remote_copy(
            src_ref=target.at[sender],
            dst_ref=target.at[sender],
            send_sem=send_sem.at[phase, k],
            recv_sem=recv_sem.at[phase, k],
            device_id={"ep": sender},
            device_id_type=MESH,
        ).wait_recv()
        return sender

    for index in range(2):
        loads[index].wait()
    x = x_v[...]
    place = (iota((heads, LANES), 0) == iota((heads, LANES), 1)).astype(jnp.bfloat16)
    step_wide = lax.dot_general(
        place, ws_v[...], (((0,), (0,)), ((), ())), preferred_element_type=jnp.float32
    ).astype(jnp.bfloat16)
    base = 2 * blocks + 2 * groups
    stage[pl.ds(base, tokens, stride=ROWS), :] = lax.dot_general(
        x, step_wide, (((1,), (1,)), ((), ())), preferred_element_type=jnp.float32
    )
    for extra in range(base + 1, ROWS):
        stage[pl.ds(extra, tokens, stride=ROWS), :] = jnp.zeros((tokens, LANES), jnp.float32)
    base = 0
    for index, ref in ((2, wg_v), (3, wv_v), (4, we_v), (5, wr_v)):
        loads[index].wait()
        product = jnp.dot(x, ref[...], preferred_element_type=jnp.float32)
        for j in range(ref.shape[1] // LANES):
            stage[pl.ds(base + j, tokens, stride=ROWS), :] = product[
                :, j * LANES : (j + 1) * LANES
            ]
        base += ref.shape[1] // LANES
    pl.semaphore_wait(barrier, n - 1)
    def token_rows(token):
        return pl.ds(pl.multiple_of(token * ROWS, ROWS), ROWS)

    parity = lax.rem(me, 2)
    exchanges = []
    for k in range(n // 2):
        copy = pltpu.make_async_remote_copy(
            src_ref=stage.at[token_rows(2 * k + 1 - parity)],
            dst_ref=pair_recv.at[k],
            send_sem=send_sem.at[6, k],
            recv_sem=recv_sem.at[6, k],
            device_id={"ep": me + 1 - 2 * parity},
            device_id_type=MESH,
        )
        copy.start()
        exchanges.append(copy)
        pending.append(copy)
    for k in range(n // 2):
        exchanges[k].wait_recv()
        own_rows = token_rows(2 * k + parity)
        stage[own_rows, :] = stage[own_rows, :] + pair_recv[k]
    post(0, lambda peer: stage.at[token_rows(peer)], part_recv, 2)

    for index in range(6, 16):
        loads[index].wait()
    old_rows = cache_v[0].astype(jnp.float32)
    tap_rows = cw_v[...].astype(jnp.float32)
    conv_blocks = tap_rows.shape[1] // LANES
    tap_count = tap_rows.shape[0]
    for j in range(conv_blocks):
        cut = slice(j * LANES, (j + 1) * LANES)
        taps[pl.ds(j, tap_count, stride=24), :] = tap_rows[:, cut]
        past[pl.ds(j, tap_count - 1, stride=24), :] = old_rows[:, cut]
    for j in range(blocks):
        gains[j : j + 1, :] = gg_v[:, j * LANES : (j + 1) * LANES]
    own_row = iota((blocks, heads), 1) // heads_a_row == iota((blocks, heads), 0)
    own_lane = (
        iota((heads, LANES), 0) % heads_a_row == iota((heads, LANES), 1) // head_dim
    ).astype(jnp.float32)

    def expand(row):
        return jnp.dot(
            jnp.where(own_row, jnp.broadcast_to(row, (blocks, heads)), 0.0),
            own_lane,
            precision=lax.Precision.HIGHEST,
            preferred_element_type=jnp.float32,
        )

    bias_rows = expand(sb_v[...])
    decay_rows = expand(dr_v[...])
    skip_rows = expand(sk_v[...])
    before = jnp.zeros((24, LANES), jnp.float32)
    for tap in range(tap_count - 1):
        before = before + past[tap * 24 : (tap + 1) * 24, :] * taps[tap * 24 : (tap + 1) * 24, :]
    last_tap = taps[(tap_count - 1) * 24 : tap_count * 24, :]
    loads[16].wait()

    total = stage[token_rows(me), :]
    for k in range(2, n, 2):
        sender = arrive(0, part_recv, k)
        total = total + part_recv[sender]
    post(1, lambda peer: x_v, x_recv)
    total = total.astype(jnp.bfloat16).astype(jnp.float32)
    fresh = total[blocks : blocks + 24, :]
    active = silu(before + fresh * last_tap)
    head_in = active[:blocks, :]
    step_row = total[2 * blocks + 2 * groups : 2 * blocks + 2 * groups + 1, :heads]
    biased = expand(step_row) + bias_rows
    step = jnp.maximum(biased, 0.0) + jnp.log1p(jnp.exp(-jnp.abs(biased)))
    retained = jnp.exp(-step * decay_rows)
    scaled_in = step * head_in
    rows_a_group = blocks // groups
    group_row = iota((blocks, 1), 0) // rows_a_group
    entry = [active[blocks + g : blocks + g + 1, :] for g in range(groups)]
    readout = [active[blocks + groups + g : blocks + groups + g + 1, :] for g in range(groups)]
    lane = iota((LANES, LANES), 1)
    columns = jnp.zeros((LANES, LANES), jnp.float32)
    for r in range(blocks):
        old = state_v[r * heads_a_row : (r + 1) * heads_a_row].reshape(LANES, LANES)
        dots = jnp.sum(old * readout[r // rows_a_group], axis=1, keepdims=True)
        columns = jnp.where(lane == r, dots, columns)
    old_out = columns.T[:blocks, :]
    cross = jnp.zeros((blocks, 1), jnp.float32)
    for g in range(groups):
        both = jnp.sum(entry[g] * readout[g], axis=1, keepdims=True)
        cross = jnp.where(group_row == g, both, cross)
    head_out = retained * old_out + scaled_in * cross + skip_rows * head_in
    gated = head_out * silu(total[:blocks, :])
    squares = jnp.sum(gated * gated, axis=1, keepdims=True)
    inverse = jnp.zeros((blocks, 1), jnp.float32)
    for g in range(groups):
        square = jnp.sum(
            jnp.where(group_row == g, squares, 0.0), axis=0, keepdims=True
        ) / (rows_a_group * LANES)
        inverse = jnp.where(group_row == g, lax.rsqrt(square + GATED_EPSILON), inverse)
    normed = (gated * inverse * gains[...]).astype(jnp.bfloat16)
    norm_send[...] = normed
    post(2, lambda peer: norm_send, norm_recv)
    norm_recv[me] = normed

    turn[0:blocks, :] = scaled_in
    turn[blocks : 2 * blocks, :] = retained
    turn[2 * blocks :, :] = jnp.zeros((LANES - 2 * blocks, LANES), jnp.float32)
    turned = turn[...].T
    for r in range(blocks):
        own = slice(r * heads_a_row, (r + 1) * heads_a_row)
        old = state_v[own].reshape(LANES, LANES)
        new = (
            turned[:, blocks + r : blocks + r + 1] * old
            + turned[:, r : r + 1] * entry[r // rows_a_group]
        )
        state_v[own] = new.reshape(heads_a_row, head_dim, LANES)
    state_out = pltpu.make_async_copy(state_v, state_ref.at[0], store_sem.at[0])
    state_out.start()
    new_row = jnp.concatenate([fresh[j : j + 1, :] for j in range(conv_blocks)], axis=1)
    conv_v[0] = jnp.concatenate([old_rows[1:, :], new_row], axis=0).astype(jnp.bfloat16)
    conv_out = pltpu.make_async_copy(conv_v, conv_ref, store_sem.at[1])
    conv_out.start()
    for index in range(17, len(moves)):
        loads[index].wait()
    x_recv[me] = x
    for k in range(1, n):
        arrive(1, x_recv, k)

    for k in range(1, n):
        arrive(2, norm_recv, k)
    for t in range(tokens):
        wide[t * blocks : (t + 1) * blocks, :] = norm_recv[t].astype(jnp.float32)
    every = jnp.concatenate(
        [wide[pl.ds(r, tokens, stride=blocks), :].astype(jnp.bfloat16) for r in range(blocks)],
        axis=1,
    )
    mixed = jnp.dot(every, ow_v[...], preferred_element_type=jnp.float32).astype(jnp.bfloat16)
    mix_send[...] = mixed
    post(3, lambda peer: mix_send, mix_recv)
    mix_recv[me] = mixed
    mine = jnp.sum(jnp.where(rt_v[...] == me, rw_v[...], 0.0), axis=0, keepdims=True)
    same = iota((tokens, tokens), 0) == iota((tokens, tokens), 1)
    mine = jnp.sum(jnp.where(same, mine, 0.0), axis=1, keepdims=True)
    for k in range(1, n):
        arrive(3, mix_recv, k)

    residuals = [
        RESIDUAL_SCALE * x_recv[d].astype(jnp.float32) + mix_recv[d].astype(jnp.float32)
        for d in range(n)
    ]
    sums = residuals[0]
    squares = residuals[0] * residuals[0]
    for d in range(1, n):
        sums = sums + residuals[d]
        squares = squares + residuals[d] * residuals[d]
    mean_value = jnp.sum(sums, axis=1, keepdims=True) / full_width
    variance = jnp.sum(squares, axis=1, keepdims=True) / full_width - mean_value * mean_value
    factor = lax.rsqrt(variance + NORM_EPSILON)
    parts = []
    for d in range(n):
        part = (
            (residuals[d] - mean_value) * factor * fg_v[:, d * LANES : (d + 1) * LANES]
        ).astype(jnp.bfloat16)
        firsts[d] = part
        parts.append(part)
    first_rows = jnp.concatenate(parts, axis=1)

    def hidden(gate_ref, up_ref):
        gate = jnp.dot(first_rows, gate_ref[...], preferred_element_type=jnp.float32)
        up = jnp.dot(first_rows, up_ref[...], preferred_element_type=jnp.float32)
        return (silu(gate) * up).astype(jnp.bfloat16)

    routed = jnp.dot(hidden(eg_v, eu_v), ed_v[...], preferred_element_type=jnp.float32)
    routed = (routed * mine).astype(jnp.bfloat16)
    for d in range(n):
        out_send[d] = routed[:, d * LANES : (d + 1) * LANES]
    post(4, lambda peer: out_send.at[peer], out_recv)
    shared = jnp.dot(hidden(sg_v, su_v), sd_v[...], preferred_element_type=jnp.float32)
    shared = shared.astype(jnp.bfloat16).astype(jnp.float32)
    moe = shared + out_send[me].astype(jnp.float32)
    for k in range(1, n):
        sender = arrive(4, out_recv, k)
        moe = moe + out_recv[sender].astype(jnp.float32)
    residual = RESIDUAL_SCALE * firsts[me].astype(jnp.float32) + moe

    row_total = jnp.sum(residual, axis=1, keepdims=True)
    row_square = jnp.sum(residual * residual, axis=1, keepdims=True)
    token = iota((tokens, LANES), 0)
    place = iota((tokens, LANES), 1)
    compact = jnp.sum(
        jnp.where(place == token, row_total, 0.0)
        + jnp.where(place == token + tokens, row_square, 0.0),
        axis=0,
        keepdims=True,
    )
    stat_send[...] = compact
    post(5, lambda peer: stat_send, stat_recv)
    for k in range(1, n):
        sender = arrive(5, stat_recv, k)
        compact = compact + stat_recv[sender]
    row_total = jnp.sum(jnp.where(place == token, compact, 0.0), axis=1, keepdims=True)
    row_square = jnp.sum(jnp.where(place == token + tokens, compact, 0.0), axis=1, keepdims=True)
    mean_value = row_total / full_width
    variance = row_square / full_width - mean_value * mean_value
    result_ref[...] = (
        (residual - mean_value) * lax.rsqrt(variance + NORM_EPSILON) * s2_v[...]
    ).astype(jnp.bfloat16)
    for copy in pending:
        copy.wait_send()
    state_out.wait()
    conv_out.wait()


CHUNKS = 4


def deliver(
    result_in,
    conv_in,
    state_in,
    result_out,
    conv_out,
    state_out,
    result_v,
    conv_v,
    state_v,
    in_sem,
    out_sem,
):
    size = state_in.shape[1] // CHUNKS
    triples = [
        tuple([r.at[0, pl.ds(c * size, size)] for r in (state_in, state_v, state_out)])
        for c in range(CHUNKS)
    ] + [(result_in, result_v, result_out), (conv_in, conv_v, conv_out)]
    reads = [
        pltpu.make_async_copy(a, v, in_sem.at[i]) for i, (a, v, _) in enumerate(triples)
    ]
    writes = [
        pltpu.make_async_copy(v, b, out_sem.at[i]) for i, (_, v, b) in enumerate(triples)
    ]
    for read in reads:
        read.start()
    for read, write in zip(reads, writes):
        read.wait()
        write.start()
    for write in writes:
        write.wait()


def fused(*arrays):
    (stream, conv_cache, scan_state) = arrays[:3]
    conv_weight = arrays[8]
    n = lax.axis_size("ep")
    inner = arrays[3].shape[1]
    groups = arrays[5].shape[1] // scan_state.shape[3]
    blocks = inner // LANES
    arrays = [a.reshape(1, -1) if a.ndim == 1 else a for a in arrays]
    for index in (7, 15, 16):
        arrays[index] = arrays[index].T
    tile = (stream.shape[0], LANES)
    landing = []
    for index, a in enumerate(arrays):
        shape = a.shape
        if index in (2, 17, 18, 19):
            shape = shape[1:]
        if index == 22:
            shape = (shape[0], LANES)
        landing.append(pltpu.VMEM(shape, a.dtype))
    bf16, f32 = jnp.bfloat16, jnp.float32
    outs = pl.pallas_call(
        functools.partial(fused_kernel, (n, inner, groups, scan_state.shape[2])),
        out_shape=(
            jax.ShapeDtypeStruct(stream.shape, bf16),
            jax.ShapeDtypeStruct(conv_cache.shape, bf16),
            jax.ShapeDtypeStruct(scan_state.shape, f32),
        ),
        in_specs=[pl.BlockSpec(memory_space=pltpu.HBM)] * len(arrays),
        out_specs=(
            pl.BlockSpec(memory_space=pltpu.VMEM),
            pl.BlockSpec(memory_space=pl.ANY),
            pl.BlockSpec(memory_space=pl.ANY),
        ),
        scratch_shapes=landing
        + [
            pltpu.VMEM(conv_cache.shape, bf16),
            pltpu.VMEM((n * ROWS, LANES), f32),
            pltpu.VMEM((n // 2, ROWS, LANES), f32),
            pltpu.VMEM((n, ROWS, LANES), f32),
            pltpu.VMEM((n,) + tile, bf16),
            pltpu.VMEM((blocks, LANES), bf16),
            pltpu.VMEM((n, blocks, LANES), bf16),
            pltpu.VMEM(tile, bf16),
            pltpu.VMEM((n,) + tile, bf16),
            pltpu.VMEM((n,) + tile, bf16),
            pltpu.VMEM((n,) + tile, bf16),
            pltpu.VMEM((1, LANES), f32),
            pltpu.VMEM((n, 1, LANES), f32),
            pltpu.VMEM((conv_weight.shape[0] * 24, LANES), f32),
            pltpu.VMEM((conv_cache.shape[1] * 24, LANES), f32),
            pltpu.VMEM((blocks, LANES), f32),
            pltpu.VMEM((LANES, LANES), f32),
            pltpu.VMEM((n * blocks, LANES), f32),
            pltpu.VMEM((n,) + tile, bf16),
            pltpu.SemaphoreType.DMA((len(arrays),)),
            pltpu.SemaphoreType.DMA((2,)),
            pltpu.SemaphoreType.DMA((7, n)),
            pltpu.SemaphoreType.DMA((7, n)),
        ],
        compiler_params=pltpu.CompilerParams(
            collective_id=0, has_side_effects=True, vmem_limit_bytes=67043328
        ),
    )(*arrays)
    return pl.pallas_call(
        deliver,
        out_shape=tuple(jax.ShapeDtypeStruct(a.shape, a.dtype) for a in outs),
        in_specs=[pl.BlockSpec(memory_space=pl.ANY)] * 3,
        out_specs=(pl.BlockSpec(memory_space=pl.ANY),) * 3,
        scratch_shapes=[pltpu.VMEM(a.shape, a.dtype) for a in outs]
        + [pltpu.SemaphoreType.DMA((2 + CHUNKS,)), pltpu.SemaphoreType.DMA((2 + CHUNKS,))],
        compiler_params=pltpu.CompilerParams(vmem_limit_bytes=67043328),
    )(*outs)


def fits(arrays):
    n = lax.axis_size("ep")
    stream, conv_cache, scan_state = arrays[:3]
    head_count, head_dim, state = scan_state.shape[1:]
    blocks = arrays[3].shape[1] // LANES
    groups = arrays[5].shape[1] // LANES
    return (
        stream.shape == (n, LANES)
        and n % 2 == 0
        and head_count % CHUNKS == 0
        and conv_cache.shape[0] == 1
        and state == LANES
        and LANES % head_dim == 0
        and head_count <= LANES
        and blocks % 8 == 0
        and 2 * blocks <= LANES
        and 2 * tokens_of(stream) <= LANES
        and blocks % groups == 0
        and arrays[8].shape[0] == conv_cache.shape[1] + 1
        and blocks + 2 * groups < 24
        and 2 * blocks + 2 * groups < ROWS
    )


def tokens_of(stream):
    return stream.shape[0]


def dispatch(*arrays):
    if fits(arrays):
        return fused(*arrays)
    return on_device(*arrays)


def solution(mesh):
    return jax.shard_map(
        dispatch,
        mesh=mesh,
        in_specs=(
            P("grp", "ep"),
            P(("grp", "ep"), None, None),
            P(("grp", "ep"), None, None, None),
            P("ep", None),
            P("ep", None),
            P("ep", None),
            P("ep", None),
            P("ep", None),
            P(),
            P(),
            P(),
            P(),
            P(),
            P(None, "ep"),
            P(),
            P("grp", None),
            P("grp", None),
            P("ep", None, None),
            P("ep", None, None),
            P("ep", None, None),
            P(),
            P(),
            P(),
            P("ep"),
        ),
        out_specs=(
            P("grp", "ep"),
            P(("grp", "ep"), None, None),
            P(("grp", "ep"), None, None, None),
        ),
        check_vma=False,
    )
```
